512 devices in a mesh: sp: 32 (over z, x), tp: 16 (over y, core).
Axes of the slice: x: 4, y: 8, z: 8, core: 2. Of those that a mesh axis runs over, the one named last changes fastest.
Arguments:
- moe_in: bfloat16 [6144, 2048], P('sp', 'tp'), may hold values from -6 to 6
- cotangent: bfloat16 [6144, 2048], P('sp', 'tp'), may hold values from -6 to 6
- routes: int32 [6144, 2], P('sp'), may hold values from 0 to 31, all different within a row; in each aligned block of 192 rows (0 to 191, 192 to 383, ...) at most 15 rows name the same one
- route_weight: float32 [6144, 2], P('sp'), may hold values from 0.2 to 1
- w_gate: bfloat16 [32, 3584, 2048], P('sp', 'tp'), may hold values from -0.125 to 0.125
- w_up: bfloat16 [32, 3584, 2048], P('sp', 'tp'), may hold values from -0.125 to 0.125
- w_down: bfloat16 [32, 3584, 2048], P('sp', 'tp'), may hold values from -0.09375 to 0.09375
- conv_pre: bfloat16 [6144, 2048], P('sp', 'tp'), may hold values from -6 to 6
- norm_mean: float32 [6144], P('sp'), may hold values from -3 to 3
- norm_rstd: float32 [6144], P('sp'), may hold values from 0.5 to 2
- ln_gain: float32 [2048], P('tp'), may hold values from 0.1 to 1.9
- ln_shift: float32 [2048], P('tp'), may hold values from -3 to 3
- taps: float32 [31, 2048], P(None, 'tp'), may hold values from -1 to 1
- w_proj: bfloat16 [2048, 2048], P('sp', 'tp'), may hold values from -0.125 to 0.125
Outputs:
- grad_up: bfloat16 [32, 3584, 2048], P('sp', 'tp')
- grad_down: bfloat16 [32, 3584, 2048], P('sp', 'tp')
- grad_stream: bfloat16 [6144, 2048], P('sp', 'tp')
- grad_proj: float32 [2048, 2048], P('sp', 'tp')
- grad_conv: bfloat16 [6144, 2048], P('sp', 'tp')
The draws below stay inside these ranges and needn't reach their ends.
Inputs may be any that keep to these rules, and one draw needn't show every extreme that they name: `routes`: each token names 2 different experts. Among the tokens of one index of sp no expert is named more than 15 times, a bound that some block reaches.
All inputs are finite; a program needn't handle non-finite values.
Results may differ from the reference program's by a relative error of at most 0.02.
Values may be sent and summed in bfloat16 or wider, within the bound.
A program may use at most 64 MiB of HBM per device.

```python
import math
import jax
import jax.numpy as jnp
import numpy as np
from jax import lax

D = 2048
FF_E = 3584
KW = 31
TOP = 2
TOK_DEV = 192
EXPERTS = 32
CAP = 15
TOKENS = 6144
N_SP = 32
N_TP = 16


def raised(drawn, key, source, target, shards_of, factor):
    owner, partner = [(jnp.arange(drawn.shape[dim]) // (drawn.shape[dim] // shards_of)).reshape([-1 if axis == dim else 1 for axis in range(drawn.ndim)]) for dim in (source, target)]
    chosen = jax.random.permutation(key, shards_of)[partner]
    strong = (owner == chosen) | (owner == (partner + shards_of // 2) % shards_of)
    return jnp.where(strong, factor * drawn, drawn)


def level_of(stream_key, shape, shards, low, top_value):
    level, own = 1.0, jax.random.fold_in(stream_key, 6)
    for position, shards_of in shards:
        heights = jnp.exp(jax.random.uniform(jax.random.fold_in(own, position), (shards_of,), jnp.float32, low / len(shards), top_value / len(shards)))
        level = level * jnp.repeat(heights, shape[position] // shards_of).reshape([-1 if axis == position else 1 for axis in range(len(shape))])
    return level


def routed_block(stream_key, own, number, rows, count, top, bound, skew):
    sequence = jax.random.permutation(stream_key, count)
    crowded, common = load_shares(count, rows * top, bound, skew, True), load_shares(count, rows * top, bound, skew, False)
    places = jnp.arange(count)

    def named(lengths, turn):
        used = int((lengths > 0).sum())
        fixed = max(1, used // 4)
        passed = fixed + (places - fixed + turn * (used - fixed)) % max(1, count - fixed)
        return jnp.zeros((count,), jnp.int32).at[sequence[jnp.where(places < fixed, places, passed)]].set(jnp.asarray(lengths, jnp.int32))

    lengths = jnp.where(number % 4 == 0, named(crowded, number // 4), named(common, number - number // 4 - 1))
    mixed = jax.random.permutation(jax.random.fold_in(own, 3), count)
    giver, sink = mixed[0:count // 2 * 2:2], mixed[1:count // 2 * 2:2]
    slack = jnp.minimum(lengths[giver] - 1, bound - lengths[sink]) // 2
    slack = jnp.where((giver == sequence[0]) | (sink == sequence[0]) | (lengths[sink] == 0), 0, jnp.maximum(slack, 0))
    passed = jax.random.randint(jax.random.fold_in(own, 4), (count // 2,), 0, 1 << 20) % (slack + 1)
    lengths = lengths.at[giver].add(-passed).at[sink].add(passed)
    members = jnp.searchsorted(jnp.cumsum(lengths), jnp.arange(rows * top), side="right").astype(jnp.int32)
    grid = members.reshape(top, rows).T
    grid = grid[jax.random.permutation(jax.random.fold_in(own, 1), rows)]
    turn = jax.random.randint(jax.random.fold_in(own, 2), (rows, 1), 0, top)
    return jnp.take_along_axis(grid, (jnp.arange(top)[None, :] + turn) % top, axis=1)


def load_shares(amount, total, limit, skew, full):
    weights = [(1 << 20) // math.isqrt(rank ** skew) + 1 for rank in range(1, amount + 1)]
    largest = limit if full else min(limit, max(-(-total // amount), total * weights[0] // sum(weights)))
    least = 1 if total - largest >= amount - 1 else 0
    given, spare = [largest] + [least] * (amount - 1), total - largest - least * (amount - 1)
    while spare > 0:
        free = [i for i in range(1, amount) if given[i] < largest] or [i for i in range(1, amount) if given[i] < limit]
        whole, left = sum([weights[i] for i in free]), spare
        for i in free:
            addition = min(limit - given[i], max(1, left * weights[i] // whole), spare)
            given[i] = given[i] + addition
            spare = spare - addition
    return np.array(given)


def normal_values(rng, shape, spread, most, shards=(), held_as=jnp.bfloat16):
    loudness = level_of(rng, shape, shards, -0.22, 0.18) if shards else 1.0
    entries = jax.random.normal(rng, shape, jnp.float32) * spread * loudness
    return jnp.minimum(jnp.maximum(entries, -most), most).astype(held_as)


def heavy_noise(stream_key, shape, deviation, bound, split, heavy, kind=jnp.bfloat16):
    entries = deviation * jax.random.normal(stream_key, shape, jnp.float32)
    if split:
        entries = entries * level_of(stream_key, shape, split, -0.22, 0.18)
    return jnp.clip(raised(entries, jax.random.fold_in(stream_key, 3), *heavy), -bound, bound).astype(kind)


def setup_inputs(seed: int = 0) -> dict:
    key_of = jax.random.split(jax.random.key(seed), 15)
    moe_in = normal_values(key_of[0], (TOKENS, D), 1.0, 6.0, ((0, 32), (1, 16)))
    cotangent = heavy_noise(key_of[1], (TOKENS, D), 1.0, 6.0, ((0, 32), (1, 16)), (0, 1, 32, 2.75))
    routes_keys = jax.random.split(jax.random.fold_in(key_of[2], 1), TOKENS // TOK_DEV)
    routes_turns = jax.random.permutation(jax.random.fold_in(key_of[2], 3), TOKENS // TOK_DEV)
    routes = jax.vmap(lambda own, number: routed_block(jax.random.fold_in(key_of[2], 2), own, number, TOK_DEV, EXPERTS, TOP, CAP, 2))(routes_keys, routes_turns).reshape((TOKENS, TOP))
    route_weight = jnp.clip(0.2 + 0.8 * jax.random.uniform(key_of[3], (TOKENS, TOP), jnp.float32) ** level_of(key_of[3], (TOKENS, TOP), ((0, 32),), -0.2, 0.2), 0.2, 1.0)
    w_gate = normal_values(key_of[4], (EXPERTS, FF_E, D), D ** -0.5, 0.125, ((0, 32), (1, 16)))
    w_up = normal_values(key_of[5], (EXPERTS, FF_E, D), D ** -0.5, 0.125, ((0, 32), (1, 16)))
    w_down = normal_values(key_of[6], (EXPERTS, FF_E, D), FF_E ** -0.5, 0.09375, ((0, 32), (1, 16)))
    conv_pre = normal_values(key_of[7], (TOKENS, D), 1.0, 6.0, ((0, 32), (1, 16)))
    norm_mean = normal_values(key_of[8], (TOKENS,), 0.5, 3.0, ((0, 32),), jnp.float32)
    norm_rstd = jnp.clip(jnp.exp(math.log(2.0) - 1.3862944 * jax.random.uniform(key_of[9], (TOKENS,), jnp.float32) ** level_of(key_of[9], (TOKENS,), ((0, 32),), -0.2, 0.2)), 0.5, 2.0)
    ln_gain = jnp.clip(1.0 + 0.18 * jax.random.normal(key_of[10], (D,), jnp.float32), 0.1, 1.9)
    ln_shift = normal_values(key_of[11], (D,), 0.5, 3.0, ((0, 16),), jnp.float32)
    taps = normal_values(key_of[12], (KW, D), KW ** -0.5, 1.0, ((1, 16),), jnp.float32)
    w_proj = normal_values(key_of[13], (D, D), D ** -0.5, 0.125, ((0, 32), (1, 16)))
    return {"moe_in": moe_in, "cotangent": cotangent, "routes": routes, "route_weight": route_weight, "w_gate": w_gate, "w_up": w_up, "w_down": w_down, "conv_pre": conv_pre, "norm_mean": norm_mean, "norm_rstd": norm_rstd, "ln_gain": ln_gain, "ln_shift": ln_shift, "taps": taps, "w_proj": w_proj}


def silu_slope(pre_value, sigmoid_value):
    return sigmoid_value * (1.0 + pre_value * (1.0 - sigmoid_value))


def expert_backward(packed):
    expert_rows, routed_rows, gate_weight, up_weight, down_weight = packed
    gate_pre = lax.dot_general(expert_rows, gate_weight, (((1,), (1,)), ((), ())), preferred_element_type=jnp.float32)
    up_pre = lax.dot_general(expert_rows, up_weight, (((1,), (1,)), ((), ())), preferred_element_type=jnp.float32)
    gate_sigmoid = jax.nn.sigmoid(gate_pre)
    gate_active = gate_pre * gate_sigmoid
    hidden = (gate_active * up_pre).astype(jnp.bfloat16)
    hidden_grad = lax.dot_general(routed_rows, down_weight, (((1,), (1,)), ((), ())), preferred_element_type=jnp.float32)
    grad_down = lax.dot_general(hidden, routed_rows, (((0,), (0,)), ((), ())), preferred_element_type=jnp.float32).astype(jnp.bfloat16)
    gate_grad = (hidden_grad * up_pre * silu_slope(gate_pre, gate_sigmoid)).astype(jnp.bfloat16)
    up_grad = (hidden_grad * gate_active).astype(jnp.bfloat16)
    grad_up = lax.dot_general(up_grad, expert_rows, (((0,), (0,)), ((), ())), preferred_element_type=jnp.float32).astype(jnp.bfloat16)
    row_count = expert_rows.shape[0]
    block_width = gate_weight.shape[0] // N_TP
    gate_blocks = gate_grad.astype(jnp.float32).reshape(row_count, N_TP, block_width)
    up_blocks = up_grad.astype(jnp.float32).reshape(row_count, N_TP, block_width)
    gate_wblocks = gate_weight.astype(jnp.float32).reshape(N_TP, block_width, D)
    up_wblocks = up_weight.astype(jnp.float32).reshape(N_TP, block_width, D)
    partial_rows = jnp.einsum("rbf,bfd->rbd", gate_blocks, gate_wblocks) + jnp.einsum("rbf,bfd->rbd", up_blocks, up_wblocks)
    partial_low = lax.optimization_barrier(partial_rows.astype(jnp.bfloat16))
    pair_grad = jnp.sum(partial_low.astype(jnp.float32), axis=1).astype(jnp.bfloat16)
    return grad_up, grad_down, pair_grad


def reference(moe_in, cotangent, routes, route_weight, w_gate, w_up, w_down, conv_pre, norm_mean, norm_rstd, ln_gain, ln_shift, taps, w_proj):
    per_expert = N_SP * CAP
    route_count = TOP * TOKENS
    route_ids = routes.reshape(N_SP, TOP * TOK_DEV)
    onehot = (route_ids[:, :, None] == jnp.arange(EXPERTS, dtype=jnp.int32)[None, None, :]).astype(jnp.int32)
    earlier = jnp.cumsum(onehot, axis=1) - onehot
    slot_ids = jnp.sum(earlier * onehot, axis=2)
    sources = jnp.arange(N_SP, dtype=jnp.int32)[:, None]
    targets = (route_ids * per_expert + sources * CAP + slot_ids).reshape(-1).astype(jnp.int32)
    table = jnp.full((EXPERTS * per_expert,), route_count, jnp.int32).at[targets].set(jnp.arange(route_count, dtype=jnp.int32))
    filled = (table < route_count)[:, None]
    route_of_slot = jnp.minimum(table, route_count - 1).astype(jnp.int32)
    routed_all = (route_weight[:, :, None] * cotangent.astype(jnp.float32)[:, None, :]).astype(jnp.bfloat16).reshape(route_count, D)
    zero_value = jnp.zeros((), jnp.bfloat16)
    expert_rows = jnp.where(filled, moe_in[route_of_slot // TOP], zero_value).reshape(EXPERTS, per_expert, D)
    routed_rows = jnp.where(filled, routed_all[route_of_slot], zero_value).reshape(EXPERTS, per_expert, D)
    grad_up, grad_down, pair_grad = lax.map(expert_backward, (expert_rows, routed_rows, w_gate, w_up, w_down))
    returned = pair_grad.reshape(EXPERTS * per_expert, D)[targets].astype(jnp.float32).reshape(TOKENS, TOP, D)
    grad_stream = (cotangent.astype(jnp.float32) + jnp.sum(returned, axis=1)).astype(jnp.bfloat16)
    normed = (conv_pre.astype(jnp.float32) - norm_mean[:, None]) * norm_rstd[:, None]
    pre_act = normed * ln_gain[None, :] + ln_shift[None, :]
    act_sigmoid = jax.nn.sigmoid(pre_act)
    activated = (pre_act * act_sigmoid).astype(jnp.bfloat16)
    act_grad = jnp.dot(grad_stream, w_proj, preferred_element_type=jnp.float32)
    grad_proj = lax.dot_general(grad_stream, activated, (((0,), (0,)), ((), ())), preferred_element_type=jnp.float32)
    normed_grad = act_grad * silu_slope(pre_act, act_sigmoid) * ln_gain[None, :]
    mean_first = jnp.mean(normed_grad, axis=1, keepdims=True)
    mean_second = jnp.mean(normed_grad * normed, axis=1, keepdims=True)
    conv_grad = norm_rstd[:, None] * (normed_grad - mean_first - normed * mean_second)
    padded = jnp.concatenate([conv_grad, jnp.zeros((KW - 1, D), jnp.float32)], axis=0)
    grad_conv = jnp.zeros((TOKENS, D), jnp.float32)
    for lag in range(KW):
        grad_conv = grad_conv + taps[lag][None, :] * padded[lag:lag + TOKENS]
    return grad_up, grad_down, grad_stream, grad_proj, grad_conv.astype(jnp.bfloat16)
```

```python
import functools

import jax
import jax.numpy as jnp
from jax import lax
from jax.experimental import pallas as pl
from jax.experimental.pallas import tpu as pltpu
from jax.sharding import PartitionSpec as P

MESH = pl.DeviceIdType.MESH
F32 = jnp.float32
BF16 = jnp.bfloat16
SLOTS = 16
NX = 4
GP = 4


def rcopy(src, dst, ssem, rsem, dev):
    return pltpu.make_async_remote_copy(
        src_ref=src, dst_ref=dst, send_sem=ssem, recv_sem=rsem, device_id=dev, device_id_type=MESH
    )


def nt(a, b):
    return lax.dot_general(a, b, (((1,), (1,)), ((), ())), preferred_element_type=F32)


def nn(a, b):
    return lax.dot_general(a, b, (((1,), (0,)), ((), ())), preferred_element_type=F32)


def tn(a, b):
    return lax.dot_general(a, b, (((0,), (0,)), ((), ())), preferred_element_type=F32)


def silu_slope(pre_value, sigmoid_value):
    return sigmoid_value * (1.0 + pre_value * (1.0 - sigmoid_value))


def sigmoid(v):
    return 1.0 / (1.0 + jnp.exp(-v))


def kernel(
    nsp,
    ntp,
    moe_ref,
    cot_ref,
    routes_ref,
    rw_ref,
    wg_hbm,
    wu_hbm,
    wd_hbm,
    conv_ref,
    mean_ref,
    rstd_ref,
    gain_ref,
    shift_ref,
    taps_ref,
    wproj_ref,
    gup_hbm,
    gdown_hbm,
    gs_out,
    gproj_out,
    gconv_out,
    pack,
    gath,
    wg,
    wu,
    wd,
    acc_g,
    acc_u,
    acc_h,
    hid,
    gg,
    ug,
    gup,
    gdown,
    mine,
    d2d_out,
    d2d_in,
    cw_in,
    ccw_in,
    cw_out,
    ccw_out,
    fin,
    back,
    wp,
    gsa,
    gp,
    gr,
    sums,
    ng_ref,
    ext,
    rim_in,
    w_sem,
    out_sem,
    a2a_s,
    a2a_r,
    nb_r,
    cw_s,
    ccw_s,
    par_s,
    par_r,
    wp_s,
    wp_r,
    d2_s,
    d2_r,
    rcw_s,
    rccw_s,
    rcw_r,
    rccw_r,
    ret_s,
    ret_r,
    gn_r,
    gcw_s,
    gccw_s,
    gpar_s,
    gpar_r,
    gp_s,
    gp_r,
    ar_s,
    ar_r,
    rim_s,
    rim_r,
):
    nz = nsp // NX
    ny = ntp // 2
    far = ny // 2
    s = lax.axis_index("sp")
    t = lax.axis_index("tp")
    z = lax.div(s, NX)
    y = lax.div(t, 2)
    c = lax.rem(t, 2)
    up_dev = (s, lax.rem(y + 1, ny) * 2 + c)
    down_dev = (s, lax.rem(y + ny - 1, ny) * 2 + c)
    pair_dev = (s, y * 2 + 1 - c)

    barrier = pltpu.get_barrier_semaphore()

    def greet_sp(i, _):
        pl.semaphore_signal(
            barrier, inc=1, device_id=(lax.rem(s + i, nsp), t), device_id_type=MESH
        )
        return 0

    def greet_tp(i, _):
        pl.semaphore_signal(
            barrier, inc=1, device_id=(s, lax.rem(t + i, ntp)), device_id_type=MESH
        )
        return 0

    lax.fori_loop(1, nsp, greet_sp, 0)
    lax.fori_loop(1, ntp, greet_tp, 0)

    w_copies = [
        pltpu.make_async_copy(wg_hbm.at[0], wg, w_sem.at[0]),
        pltpu.make_async_copy(wu_hbm.at[0], wu, w_sem.at[1]),
        pltpu.make_async_copy(wd_hbm.at[0], wd, w_sem.at[2]),
    ]
    for copy in w_copies:
        copy.start()

    tok = moe_ref.shape[0]
    slots = nsp * SLOTS
    eye = lax.broadcasted_iota(jnp.int32, (tok, tok), 0) == lax.broadcasted_iota(
        jnp.int32, (tok, tok), 1
    )
    before = lax.broadcasted_iota(jnp.int32, (tok, tok), 1) < lax.broadcasted_iota(
        jnp.int32, (tok, tok), 0
    )
    expert_lane = lax.broadcasted_iota(jnp.int32, (tok, 128), 1)
    hot = [(routes_ref[:, k : k + 1] == expert_lane).astype(F32) for k in range(2)]
    counts = nn(
        jnp.where(before, 1.0, 0.0).astype(BF16), (hot[0] + hot[1]).astype(BF16)
    )
    target_col = [
        jnp.sum(hot[k] * counts, axis=1, keepdims=True)
        + SLOTS * routes_ref[:, k : k + 1].astype(F32)
        for k in range(2)
    ]
    slot_row = lax.broadcasted_iota(jnp.int32, (slots, tok), 0).astype(F32)
    place = [
        jnp.where(
            slot_row == jnp.sum(jnp.where(eye, target_col[k], 0.0), axis=0, keepdims=True), 1.0, 0.0
        ).astype(BF16)
        for k in range(2)
    ]
    cot = cot_ref[...]
    cot_f = cot.astype(F32)
    rows = nn(place[0] + place[1], moe_ref[...])
    weighted = nn(place[0], (rw_ref[:, 0:1] * cot_f).astype(BF16)) + nn(
        place[1], (rw_ref[:, 1:2] * cot_f).astype(BF16)
    )
    pack[:, 0:SLOTS, :] = rows.astype(BF16).reshape(nsp, SLOTS, 128)
    pack[:, SLOTS : 2 * SLOTS, :] = weighted.astype(BF16).reshape(nsp, SLOTS, 128)

    pl.semaphore_wait(barrier, nsp + ntp - 2)

    def dz(k):
        odd = lax.rem(k, 2)
        return odd * lax.div(k + 1, 2) + (1 - odd) * lax.rem(nz - lax.div(k, 2), nz)

    def peer(k, i):
        return lax.rem(z + dz(k), nz) * NX + lax.rem(s + i, NX)

    def send_rows(k, _):
        for i in range(NX):
            e = peer(k, i)

            @pl.when(e != s)
            def _():
                rcopy(pack.at[e], gath.at[t, s], a2a_s.at[e], a2a_r.at[s], (e, t)).start()

        return 0

    lax.fori_loop(0, nz, send_rows, 0)
    gath[t, s] = pack[s]

    def part_of(r):
        return lax.rem(y + ny - r, ny) * 2 + c

    def piece(r, k):
        zs = lax.rem(z + nz - dz(k), nz)
        return gath.at[part_of(r), pl.ds(zs * NX, NX)]

    def to_up(r, k):
        return rcopy(piece(r, k), piece(r, k), cw_s.at[r, k], nb_r.at[r + 1, k], up_dev)

    def to_down(r, k):
        return rcopy(
            piece(r, k), piece(r, k), ccw_s.at[r, k], nb_r.at[(r + ny - 1) % ny, k], down_dev
        )

    def to_pair(r, k):
        return rcopy(piece(r, k), piece(r, k), par_s.at[r, k], par_r.at[r, k], pair_dev)

    def from_nb(r, k):
        rcopy(piece(r, k), piece(r, k), cw_s.at[r, k], nb_r.at[r, k], up_dev).wait_recv()

    def own_stage(k, _):
        zs = lax.rem(z + nz - dz(k), nz)
        for i in range(NX):
            e = zs * NX + i

            @pl.when(e != s)
            def _():
                rcopy(pack.at[e], gath.at[t, e], a2a_s.at[e], a2a_r.at[e], (e, t)).wait_recv()

        to_up(0, k).start()
        to_down(0, k).start()
        to_pair(0, k).start()
        return 0

    lax.fori_loop(0, nz, own_stage, 0)

    def send_wp(k, _):
        for i in range(NX):
            e = peer(k, i)

            @pl.when(e != s)
            def _():
                rcopy(wproj_ref, wp.at[s], wp_s.at[e], wp_r.at[s], (e, t)).start()

        return 0

    lax.fori_loop(0, nz, send_wp, 0)
    wp[s] = wproj_ref[...]

    acc_g[...] = jnp.zeros_like(acc_g)
    acc_u[...] = jnp.zeros_like(acc_u)
    acc_h[...] = jnp.zeros_like(acc_h)
    for copy in w_copies:
        copy.wait()

    def stage(h):
        def body(kk, _):
            for odd in range(2):
                k = 2 * kk + odd
                for cw in (True, False):
                    reach = far if cw != bool(odd) else ny - 1 - far
                    if h > reach:
                        continue
                    r = h if cw else ny - h
                    from_nb(r, k)
                    if h < reach:
                        (to_up(r, k) if cw else to_down(r, k)).start()
                    to_pair(r, k).start()
            return 0

        lax.fori_loop(0, nz // 2, body, 0)

    def chip_rows(yp, lo):
        return jnp.concatenate(
            [
                gath[2 * yp, :, lo : lo + SLOTS, :].reshape(slots, 128),
                gath[2 * yp + 1, :, lo : lo + SLOTS, :].reshape(slots, 128),
            ],
            axis=1,
        )

    def contract(rs):
        def one(r):
            def arrived(k, _):
                rcopy(
                    piece(r, k),
                    gath.at[
                        lax.rem(y + ny - r, ny) * 2 + 1 - c,
                        pl.ds(lax.rem(z + nz - dz(k), nz) * NX, NX),
                    ],
                    par_s.at[r, k],
                    par_r.at[r, k],
                    pair_dev,
                ).wait_recv()
                return 0

            lax.fori_loop(0, nz, arrived, 0)
            yp = lax.rem(y + ny - r, ny)
            cols = pl.ds(pl.multiple_of(yp * 256, 256), 256)
            a = chip_rows(yp, 0)
            acc_g[...] += nt(a, wg[:, cols])
            acc_u[...] += nt(a, wu[:, cols])
            acc_h[...] += nt(chip_rows(yp, SLOTS), wd[:, cols])

        for r in rs:
            one(r)

    for h in range(1, far + 1):
        stage(h)
        contract([0] if h == 1 else [h - 1, ny - h + 1])
    contract([far])

    gate_pre = acc_g[...]
    up_pre = acc_u[...]
    hidden_grad = acc_h[...]
    gate_sig = sigmoid(gate_pre)
    gate_active = gate_pre * gate_sig
    gg[...] = (hidden_grad * up_pre * silu_slope(gate_pre, gate_sig)).astype(BF16)
    ug[...] = (hidden_grad * gate_active).astype(BF16)
    hid[...] = (gate_active * up_pre).astype(BF16)

    def to_partner(d):
        return rcopy(d2d_out.at[d], d2d_in.at[d], d2_s.at[d], d2_r.at[d], pair_dev)

    def partials(ds):
        for d in ds:
            yp = lax.rem(y + d, ny)
            cols = pl.ds(pl.multiple_of(yp * 256, 256), 256)
            both = nn(gg[...], wg[:, cols]) + nn(ug[...], wu[:, cols])
            first, second = both[:, :128], both[:, 128:]
            mine[d] = jnp.where(c == 0, first, second)
            d2d_out[d] = jnp.where(c == 0, second, first).astype(BF16)
            to_partner(d).start()

    row_count = NX * SLOTS

    def block(k):
        zd = lax.rem(z + dz(k), nz)
        return pl.ds(pl.multiple_of(zd * row_count, row_count), row_count)

    def ring(d):
        def body(kk, _):
            for odd in range(2):
                k = 2 * kk + odd
                at = block(k)
                for cw in (True, False):
                    reach = far if cw != bool(odd) else ny - 1 - far
                    if d > reach:
                        continue
                    rel = d if cw else ny - d
                    got, out = (cw_in, cw_out) if cw else (ccw_in, ccw_out)
                    ssem, rsem = (rcw_s, rcw_r) if cw else (rccw_s, rccw_r)
                    dev = up_dev if cw else down_dev
                    val = mine[rel, at, :] + d2d_in[rel, at, :].astype(F32)
                    if d < reach:
                        rcopy(
                            out.at[d, at], got.at[d, at], ssem.at[d, k], rsem.at[d, k], dev
                        ).wait_recv()
                        val = val + got[d, at, :].astype(F32)
                    out[d, at, :] = val.astype(BF16)
                    rcopy(
                        out.at[d, at], got.at[d - 1, at], ssem.at[d, k], rsem.at[d - 1, k], dev
                    ).start()
            return 0

        lax.fori_loop(0, nz // 2, body, 0)

    def pair_ready(ds):
        for d in ds:
            to_partner(d).wait_recv()

    partials([far])
    partials([far - 1, ny - far + 1])
    pair_ready([far])
    ring(far)
    for d in range(far - 1, 0, -1):
        partials([d - 1] if d == 1 else [d - 1, ny - d + 1])
        pair_ready([d, ny - d])
        ring(d)
    pair_ready([0])

    def finish(k, _):
        at = block(k)
        rcopy(cw_out.at[1, at], cw_in.at[0, at], rcw_s.at[1, k], rcw_r.at[0, k], up_dev).wait_recv()
        rcopy(
            ccw_out.at[1, at], ccw_in.at[0, at], rccw_s.at[1, k], rccw_r.at[0, k], down_dev
        ).wait_recv()
        val = (
            mine[0, at, :]
            + d2d_in[0, at, :].astype(F32)
            + cw_in[0, at, :].astype(F32)
            + ccw_in[0, at, :].astype(F32)
        )
        zd = lax.rem(z + dz(k), nz)
        fin[pl.ds(zd * NX, NX)] = val.astype(BF16).reshape(NX, SLOTS, 128)
        for i in range(NX):
            e = peer(k, i)

            @pl.when(e != s)
            def _():
                rcopy(fin.at[e], back.at[s], ret_s.at[e], ret_r.at[s], (e, t)).start()

        return 0

    lax.fori_loop(0, nz, finish, 0)
    back[s] = fin[s]

    hid_t = hid[...].T
    ug_t = ug[...].T

    def weight_grads(yp, _):
        cols = pl.ds(pl.multiple_of(yp * 256, 256), 256)
        gdown[:, cols] = nn(hid_t, chip_rows(yp, SLOTS)).astype(BF16)
        gup[:, cols] = nn(ug_t, chip_rows(yp, 0)).astype(BF16)
        return 0

    lax.fori_loop(0, ny, weight_grads, 0)
    out_copies = [
        pltpu.make_async_copy(gup, gup_hbm.at[0], out_sem.at[0]),
        pltpu.make_async_copy(gdown, gdown_hbm.at[0], out_sem.at[1]),
    ]
    for copy in out_copies:
        copy.start()

    normed = (conv_ref[...].astype(F32) - mean_ref[...]) * rstd_ref[...]
    pre_act = normed * gain_ref[...] + shift_ref[...]
    act_sig = sigmoid(pre_act)
    activated = (pre_act * act_sig).astype(BF16)
    slope = silu_slope(pre_act, act_sig) * gain_ref[...]

    def returned(e, _):
        @pl.when(e != s)
        def _():
            rcopy(fin.at[e], back.at[e], ret_s.at[e], ret_r.at[e], (e, t)).wait_recv()

        return 0

    lax.fori_loop(0, nsp, returned, 0)
    slot_lane = lax.broadcasted_iota(jnp.int32, (tok, slots), 1).astype(F32)
    pick = jnp.where((slot_lane == target_col[0]) | (slot_lane == target_col[1]), 1.0, 0.0)
    grad_stream = (cot_f + nn(pick.astype(BF16), back[...].reshape(slots, 128))).astype(BF16)
    gs_out[...] = grad_stream
    gsa[t] = grad_stream

    step = tok // GP

    def gpiece(r, k, other=False):
        part = lax.rem(y + ny - r, ny) * 2 + (1 - c if other else c)
        return gsa.at[part, pl.ds(k * step, step)]

    def g_up(r, k):
        return rcopy(gpiece(r, k), gpiece(r, k), gcw_s.at[r, k], gn_r.at[r + 1, k], up_dev)

    def g_down(r, k):
        return rcopy(
            gpiece(r, k), gpiece(r, k), gccw_s.at[r, k], gn_r.at[(r + ny - 1) % ny, k], down_dev
        )

    def g_pair(r, k):
        return rcopy(gpiece(r, k), gpiece(r, k), gpar_s.at[r, k], gpar_r.at[r, k], pair_dev)

    def g_from(r, k):
        rcopy(gpiece(r, k), gpiece(r, k), gcw_s.at[r, k], gn_r.at[r, k], up_dev).wait_recv()

    for k in range(GP):
        g_up(0, k).start()
        g_down(0, k).start()
        g_pair(0, k).start()

    def wp_arrived(e, _):
        @pl.when(e != s)
        def _():
            rcopy(wproj_ref, wp.at[e], wp_s.at[e], wp_r.at[e], (e, t)).wait_recv()

        return 0

    lax.fori_loop(0, nsp, wp_arrived, 0)
    w_rows = wp.shape[1]
    chunk = 256 // w_rows

    def g_stage(h):
        for k in range(GP):
            for cw in (True, False):
                reach = far if cw != bool(k % 2) else ny - 1 - far
                if h > reach:
                    continue
                r = h if cw else ny - h
                g_from(r, k)
                if h < reach:
                    (g_up(r, k) if cw else g_down(r, k)).start()
                g_pair(r, k).start()

    def g_contract(rs, total):
        for r in rs:
            for k in range(GP):
                rcopy(
                    gpiece(r, k), gpiece(r, k, True), gpar_s.at[r, k], gpar_r.at[r, k], pair_dev
                ).wait_recv()
            yp = lax.rem(y + ny - r, ny)
            a = jnp.concatenate([gsa[2 * yp], gsa[2 * yp + 1]], axis=1)
            total = total + nn(a, wp[pl.ds(yp * chunk, chunk)].reshape(256, 128))
            gp[pl.ds(yp * chunk, chunk)] = tn(a, activated).astype(BF16).reshape(
                chunk, w_rows, 128
            )
        return total

    act_grad = jnp.zeros((tok, 128), F32)
    for h in range(1, far + 1):
        g_stage(h)
        act_grad = g_contract([0] if h == 1 else [h - 1, ny - h + 1], act_grad)
    act_grad = g_contract([far], act_grad)

    ng = act_grad * slope
    ng_n = ng * normed
    ones = jnp.ones((8, 128), F32)

    def row_sums(v):
        return lax.dot_general(
            ones,
            v,
            (((1,), (1,)), ((), ())),
            preferred_element_type=F32,
            precision=lax.Precision.HIGHEST,
        )[0:1]

    sums[t] = jnp.concatenate([row_sums(ng), row_sums(ng_n)], axis=0)

    def send_sums(i, _):
        o = lax.rem(t + i, ntp)
        rcopy(sums.at[t], sums.at[t], ar_s.at[o], ar_r.at[t], (s, o)).start()
        return 0

    lax.fori_loop(1, ntp, send_sums, 0)

    def send_gp(k, _):
        for i in range(NX):
            e = peer(k, i)

            @pl.when(e != s)
            def _():
                rcopy(gp.at[e], gr.at[s], gp_s.at[e], gp_r.at[s], (e, t)).start()

        return 0

    lax.fori_loop(0, nz, send_gp, 0)
    gr[s] = gp[s]

    def sums_arrived(i, _):
        o = lax.rem(t + i, ntp)
        rcopy(sums.at[o], sums.at[o], ar_s.at[o], ar_r.at[o], (s, o)).wait_recv()
        return 0

    lax.fori_loop(1, ntp, sums_arrived, 0)
    total = jnp.sum(sums[...], axis=0) * (1.0 / (ntp * 128))
    mean_col = [
        jnp.sum(jnp.where(eye, total[k : k + 1, :], 0.0), axis=1, keepdims=True) for k in range(2)
    ]
    conv_grad = rstd_ref[...] * (ng - mean_col[0] - normed * mean_col[1])
    ext[0:tok, :] = conv_grad

    prev_dev = (lax.rem(s + nsp - 1, nsp), t)
    rim = rcopy(ext.at[pl.ds(0, 32)], rim_in, rim_s, rim_r, prev_dev)
    rim.start()
    rim.wait_recv()
    ext[tok : tok + 32, :] = jnp.where(s == nsp - 1, 0.0, rim_in[...])
    conv = jnp.zeros((tok, 128), F32)
    for lag in range(taps_ref.shape[0]):
        conv = conv + taps_ref[lag : lag + 1, :] * ext[lag : lag + tok, :]
    gconv_out[...] = conv.astype(BF16)

    def gp_arrived(e, _):
        @pl.when(e != s)
        def _():
            rcopy(gp.at[e], gr.at[e], gp_s.at[e], gp_r.at[e], (e, t)).wait_recv()

        return 0

    lax.fori_loop(0, nsp, gp_arrived, 0)

    def add_gp(e, v):
        return v + gr[e].astype(F32)

    gproj_out[...] = lax.fori_loop(0, nsp, add_gp, jnp.zeros((w_rows, 128), F32))

    rim.wait_send()
    for copy in out_copies:
        copy.wait()

    def drain_sp(e, _):
        @pl.when(e != s)
        def _():
            rcopy(pack.at[e], gath.at[t, s], a2a_s.at[e], a2a_r.at[s], (e, t)).wait_send()
            rcopy(wproj_ref, wp.at[s], wp_s.at[e], wp_r.at[s], (e, t)).wait_send()
            rcopy(fin.at[e], back.at[s], ret_s.at[e], ret_r.at[s], (e, t)).wait_send()
            rcopy(gp.at[e], gr.at[s], gp_s.at[e], gp_r.at[s], (e, t)).wait_send()

        return 0

    lax.fori_loop(0, nsp, drain_sp, 0)

    def drain_tp(i, _):
        o = lax.rem(t + i, ntp)
        rcopy(sums.at[t], sums.at[t], ar_s.at[o], ar_r.at[t], (s, o)).wait_send()
        return 0

    lax.fori_loop(1, ntp, drain_tp, 0)
    for d in range(ny):
        to_partner(d).wait_send()

    def drain_pieces(kk, _):
        for odd in range(2):
            k = 2 * kk + odd
            at = block(k)
            for r in range(ny):
                to_pair(r, k).wait_send()
            for cw in (True, False):
                reach = far if cw != bool(odd) else ny - 1 - far
                for h in range(reach):
                    r = h if cw else (ny - h) % ny
                    (to_up(r, k) if cw else to_down(r, k)).wait_send()
                for d in range(1, reach + 1):
                    if cw:
                        rcopy(
                            cw_out.at[d, at], cw_in.at[d - 1, at], rcw_s.at[d, k], rcw_r.at[d - 1, k], up_dev
                        ).wait_send()
                    else:
                        rcopy(
                            ccw_out.at[d, at], ccw_in.at[d - 1, at], rccw_s.at[d, k], rccw_r.at[d - 1, k], down_dev
                        ).wait_send()
        return 0

    lax.fori_loop(0, nz // 2, drain_pieces, 0)
    for k in range(GP):
        for r in range(ny):
            g_pair(r, k).wait_send()
        for cw in (True, False):
            reach = far if cw != bool(k % 2) else ny - 1 - far
            for h in range(reach):
                r = h if cw else (ny - h) % ny
                (g_up(r, k) if cw else g_down(r, k)).wait_send()


def on_device(
    moe_in,
    cotangent,
    routes,
    route_weight,
    w_gate,
    w_up,
    w_down,
    conv_pre,
    norm_mean,
    norm_rstd,
    ln_gain,
    ln_shift,
    taps,
    w_proj,
):
    nsp = lax.axis_size("sp")
    ntp = lax.axis_size("tp")
    nz = nsp // NX
    ny = ntp // 2
    far = ny // 2
    tok = moe_in.shape[0]
    ff, width = w_gate.shape[1:]
    slots = nsp * SLOTS
    w_rows = w_proj.shape[0]
    vmem = pl.BlockSpec(memory_space=pltpu.VMEM)
    hbm = pl.BlockSpec(memory_space=pl.ANY)
    dma = pltpu.SemaphoreType.DMA
    return pl.pallas_call(
        functools.partial(kernel, nsp, ntp),
        out_shape=(
            jax.ShapeDtypeStruct(w_up.shape, BF16),
            jax.ShapeDtypeStruct(w_down.shape, BF16),
            jax.ShapeDtypeStruct((tok, 128), BF16),
            jax.ShapeDtypeStruct((w_rows, 128), F32),
            jax.ShapeDtypeStruct((tok, 128), BF16),
        ),
        in_specs=[vmem] * 4 + [hbm] * 3 + [vmem] * 7,
        out_specs=(hbm, hbm, vmem, vmem, vmem),
        scratch_shapes=[
            pltpu.VMEM((nsp, 2 * SLOTS, 128), BF16),
            pltpu.VMEM((ntp, nsp, 2 * SLOTS, 128), BF16),
            pltpu.VMEM((ff, width), BF16),
            pltpu.VMEM((ff, width), BF16),
            pltpu.VMEM((ff, width), BF16),
            pltpu.VMEM((slots, ff), F32),
            pltpu.VMEM((slots, ff), F32),
            pltpu.VMEM((slots, ff), F32),
            pltpu.VMEM((slots, ff), BF16),
            pltpu.VMEM((slots, ff), BF16),
            pltpu.VMEM((slots, ff), BF16),
            pltpu.VMEM((ff, width), BF16),
            pltpu.VMEM((ff, width), BF16),
            pltpu.VMEM((ny, slots, 128), F32),
            pltpu.VMEM((ny, slots, 128), BF16),
            pltpu.VMEM((ny, slots, 128), BF16),
            pltpu.VMEM((far, slots, 128), BF16),
            pltpu.VMEM((far, slots, 128), BF16),
            pltpu.VMEM((far + 1, slots, 128), BF16),
            pltpu.VMEM((far + 1, slots, 128), BF16),
            pltpu.VMEM((nsp, SLOTS, 128), BF16),
            pltpu.VMEM((nsp, SLOTS, 128), BF16),
            pltpu.VMEM((nsp, w_rows, 128), BF16),
            pltpu.VMEM((ntp, tok, 128), BF16),
            pltpu.VMEM((nsp, w_rows, 128), BF16),
            pltpu.VMEM((nsp, w_rows, 128), BF16),
            pltpu.VMEM((ntp, 2, tok), F32),
            pltpu.VMEM((tok, 128), F32),
            pltpu.VMEM((tok + 32, 128), F32),
            pltpu.VMEM((32, 128), F32),
            dma((3,)),
            dma((2,)),
            dma((nsp,)),
            dma((nsp,)),
            dma((ny, nz)),
            dma((ny, nz)),
            dma((ny, nz)),
            dma((ny, nz)),
            dma((ny, nz)),
            dma((nsp,)),
            dma((nsp,)),
            dma((ny,)),
            dma((ny,)),
            dma((far + 1, nz)),
            dma((far + 1, nz)),
            dma((far, nz)),
            dma((far, nz)),
            dma((nsp,)),
            dma((nsp,)),
            dma((ny, GP)),
            dma((ny, GP)),
            dma((ny, GP)),
            dma((ny, GP)),
            dma((ny, GP)),
            dma((nsp,)),
            dma((nsp,)),
            dma((ntp,)),
            dma((ntp,)),
            dma,
            dma,
        ],
        compiler_params=pltpu.CompilerParams(
            collective_id=0, has_side_effects=True, vmem_limit_bytes=60 * 1024 * 1024
        ),
        name="layer_backward",
    )(
        moe_in,
        cotangent,
        routes,
        route_weight,
        w_gate,
        w_up,
        w_down,
        conv_pre,
        norm_mean[:, None],
        norm_rstd[:, None],
        ln_gain[None, :],
        ln_shift[None, :],
        taps,
        w_proj,
    )


def solution(mesh):
    placed = (
        P("sp", "tp"),
        P("sp", "tp"),
        P("sp", None),
        P("sp", None),
        P("sp", "tp", None),
        P("sp", "tp", None),
        P("sp", "tp", None),
        P("sp", "tp"),
        P("sp"),
        P("sp"),
        P("tp"),
        P("tp"),
        P(None, "tp"),
        P("sp", "tp"),
    )
    return jax.shard_map(
        on_device,
        mesh=mesh,
        in_specs=placed,
        out_specs=(
            P("sp", "tp", None),
            P("sp", "tp", None),
            P("sp", "tp"),
            P("sp", "tp"),
            P("sp", "tp"),
        ),
        check_vma=False,
    )
```
